32 devices in a mesh: kv: 8 (over z, y), tp: 4 (over x, core).
Axes of the slice: x: 2, y: 2, z: 4, core: 2. Of those that a mesh axis runs over, the one named last changes fastest.
Arguments:
- activations: bfloat16 [2048, 4096], P('kv'), may hold values from -14 to 14
- query_weight: bfloat16 [4096, 2048], P(None, 'tp'), may hold values from -0.09375 to 0.09375
- key_weight: bfloat16 [4096, 256], P(None, 'tp'), may hold values from -0.09375 to 0.09375
- value_weight: bfloat16 [4096, 256], P(None, 'tp'), may hold values from -0.09375 to 0.09375
- chosen: int32 [16, 16], P('kv'), may hold values from 0 to 63, as said below
- out_gain: float32 [2048], replicated, may hold values from 0.1 to 1.9
- out_weight: bfloat16 [2048, 4096], P(None, 'tp'), may hold values from -0.125 to 0.125
Outputs:
- mixed: bfloat16 [2048, 4096], P('kv', 'tp')
The draws below stay inside these ranges and needn't reach their ends.
Inputs may be any that keep to these rules, and one draw needn't show every extreme that they name: `chosen`: the first 4 entries of a row name the key blocks of that row's own query block; every entry names a key block that ends no later than its query block; a block may be named more than once in a row.
All inputs are finite; a program needn't handle non-finite values.
Results may differ from the reference program's by a relative error of at most 0.012.
The reference program's roundings to bfloat16 on the way count: a program that leaves them out, or rounds other values in their place, can miss the bound.
Values may be sent and summed in bfloat16 or wider, within the bound.
No kernel may reach another device: no remote copies, remote signals or barrier semaphores. Data moves between devices by JAX's collectives and lax.ppermute only.
A program may use at most 64 MiB of HBM per device.

```python
import math
import jax
import jax.numpy as jnp
from jax import lax

D = 4096
HEADS = 16
HD = 128
KVH = 2
TOK_DEV = 256
QB = 128
KB = 32
SEL = 16
TOKENS = 2048


def draw_activations(key, part):
    base_key = jax.random.fold_in(key, 11)
    drawn = jnp.clip(jax.random.normal(base_key, (TOKENS, D), jnp.float32), -5.0, 5.0)
    return drawn.astype(jnp.bfloat16)


def draw_chosen(key, part):
    query_blocks = TOKENS // QB
    own_count = QB // KB
    device_blocks = TOK_DEV // KB
    devices = TOKENS // TOK_DEV
    half_axis = devices // 2
    query_block = jnp.arange(query_blocks, dtype=jnp.int32)
    owner = query_block // (TOK_DEV // QB)
    first_own = query_block * own_count
    last_own = first_own + own_count - 1
    own_blocks = first_own[:, None] + jnp.arange(own_count, dtype=jnp.int32)[None, :]
    prior_selection = jax.random.randint(jax.random.fold_in(key, 21), (query_blocks,), 0, device_blocks)
    before = jnp.where(owner >= 1, (owner - 1) * device_blocks + prior_selection, last_own)
    far_pick = jax.random.randint(jax.random.fold_in(key, 22), (query_blocks,), 0, device_blocks)
    far_block = jnp.where(owner >= half_axis, (owner - half_axis) * device_blocks + far_pick, last_own)
    rest_count = SEL - own_count - 2
    popular = jax.random.randint(jax.random.fold_in(key, 23), (8,), 0, TOKENS // KB)
    which_popular = jax.random.randint(jax.random.fold_in(key, 24), (query_blocks, rest_count), 0, 8)
    coin_flip = jax.random.randint(jax.random.fold_in(key, 25), (query_blocks, rest_count), 0, 2)
    spread = jax.random.randint(jax.random.fold_in(key, 26), (query_blocks, rest_count), 0, 1073741824)
    spread = spread % (last_own[:, None] + 1)
    favored = popular[which_popular]
    picked_rest = jnp.where((coin_flip == 0) & (favored <= last_own[:, None]), favored, spread)
    merged = jnp.concatenate([own_blocks, before[:, None], far_block[:, None], picked_rest], axis=1)
    return merged.astype(jnp.int32)


def levels(stream_key, dims, cuts, low, high):
    factor_of, own = 1.0, jax.random.fold_in(stream_key, 6)
    for axis_at, shards_of in cuts:
        draws = jnp.exp(jax.random.uniform(jax.random.fold_in(own, axis_at), (shards_of,), jnp.float32, low / len(cuts), high / len(cuts)))
        factor_of = factor_of * jnp.repeat(draws, dims[axis_at] // shards_of).reshape([-1 if axis == axis_at else 1 for axis in range(len(dims))])
    return factor_of


def gaussian(key, extent, scale, most, cuts=(), kind=jnp.bfloat16):
    result = scale * jax.random.normal(key, extent, jnp.float32)
    if cuts:
        result = result * levels(key, extent, cuts, -0.22, 0.18)
    return jnp.clip(result, -most, most).astype(kind)


def setup_inputs(seed: int = 0) -> dict:
    streams_of = jax.random.split(jax.random.key(seed), 8)
    return {
        "activations": draw_activations(jax.random.fold_in(streams_of[7], 71), 0),
        "query_weight": gaussian(streams_of[1], (D, HEADS * HD), D ** -0.5, 0.09375, ((1, 4),)),
        "key_weight": gaussian(streams_of[2], (D, KVH * HD), D ** -0.5, 0.09375, ((1, 4),)),
        "value_weight": gaussian(streams_of[3], (D, KVH * HD), D ** -0.5, 0.09375, ((1, 4),)),
        "chosen": draw_chosen(jax.random.fold_in(streams_of[7], 71), 0),
        "out_gain": jnp.clip(1.0 + 0.18 * jax.random.normal(streams_of[5], (HEADS * HD,), jnp.float32), 0.1, 1.9),
        "out_weight": gaussian(streams_of[6], (HEADS * HD, D), (HEADS * HD) ** -0.5, 0.125, ((1, 4),)),
    }


def reference(activations, query_weight, key_weight, value_weight, chosen, out_gain, out_weight):
    queries = jnp.dot(activations, query_weight, preferred_element_type=jnp.float32).astype(jnp.bfloat16)
    keys = jnp.dot(activations, key_weight, preferred_element_type=jnp.float32).astype(jnp.bfloat16)
    values = jnp.dot(activations, value_weight, preferred_element_type=jnp.float32).astype(jnp.bfloat16)
    key_blocks = keys.reshape(TOKENS // KB, KB, KVH * HD)
    value_blocks = values.reshape(TOKENS // KB, KB, KVH * HD)
    group_size = HEADS // KVH
    score_scale = 1.0 / math.sqrt(HD)
    offsets = jnp.arange(KB, dtype=jnp.int32)
    preceding_mask = jnp.arange(SEL)[None, :] < jnp.arange(SEL)[:, None]

    def one_block(block_index):
        picked = chosen[block_index]
        repeats = picked[:, None] == picked[None, :]
        fresh = jnp.logical_not(jnp.any(repeats & preceding_mask, axis=1))
        key_pos = (picked[:, None] * KB + offsets[None, :]).reshape(SEL * KB)
        key_fresh = jnp.repeat(fresh, KB)
        query_pos = block_index * QB + jnp.arange(QB, dtype=jnp.int32)
        allowed = key_fresh[None, :] & (key_pos[None, :] <= query_pos[:, None])
        block_keys = key_blocks[picked].reshape(SEL * KB, KVH, HD).astype(jnp.float32)
        block_values = value_blocks[picked].reshape(SEL * KB, KVH, HD).astype(jnp.float32)
        query_block_rows = lax.dynamic_slice_in_dim(queries, block_index * QB, QB, 0)
        query_block_rows = query_block_rows.reshape(QB, group_size, KVH, HD).astype(jnp.float32)
        scores = jnp.einsum('qmgd,kgd->qmgk', query_block_rows, block_keys) * score_scale
        scores = jnp.where(allowed[:, None, None, :], scores, -jnp.inf)
        row_peak = lax.optimization_barrier(jnp.max(scores, axis=3, keepdims=True))
        attention_weight = jnp.exp(scores - row_peak)
        attention_weight = (attention_weight / lax.optimization_barrier(jnp.sum(attention_weight, axis=3, keepdims=True))).astype(jnp.bfloat16)
        block_out = jnp.einsum('qmgk,kgd->qmgd', attention_weight.astype(jnp.float32), block_values)
        return block_out.astype(jnp.bfloat16).reshape(QB, HEADS * HD)
    attention_result = lax.map(one_block, jnp.arange(TOKENS // QB, dtype=jnp.int32)).reshape(TOKENS, HEADS * HD)
    row_energy = lax.optimization_barrier(jnp.sum(jnp.square(attention_result.astype(jnp.float32)), axis=1))
    row_scale = lax.rsqrt(row_energy / (HEADS * HD) + 1e-06)
    gained = (attention_result.astype(jnp.float32) * out_gain.astype(jnp.float32)).astype(jnp.bfloat16)
    projected = jnp.dot(gained, out_weight, preferred_element_type=jnp.float32)
    return (projected * row_scale[:, None]).astype(jnp.bfloat16)
```

```python
import functools
import math

import jax
import jax.numpy as jnp
from jax import lax
from jax.experimental import pallas as pl
from jax.experimental.pallas import tpu as pltpu
from jax.sharding import PartitionSpec as P

HD = 128
KVH = 2
QB = 128
KB = 32
SEL = 16
FAR = 2**30


VMEM = pl.BlockSpec(memory_space=pltpu.VMEM)
SMEM = pl.BlockSpec(memory_space=pltpu.SMEM)


def gather_before(part, n):
    if n > 16:
        every = lax.all_gather(part, "kv", axis=0, tiled=False)
        at = (lax.axis_index("kv") - jnp.arange(n, dtype=jnp.int32)) % n
        return [jnp.take(every, at, axis=0).reshape(-1, part.shape[1])]
    return [part] + [
        lax.ppermute(part, "kv", [(i, (i + s) % n) for i in range(n)]) for s in range(1, n)
    ]


def swap(x, n, s):
    return lax.ppermute(x, "tp", [(i, i ^ s) for i in range(n)])


def select_kernel(where_ref, chosen_ref, *refs, pieces, group, rows, tok):
    ins, outs, all_ref = refs[:pieces], refs[pieces : pieces + group], refs[-1]
    kv, r = where_ref[0], where_ref[2]
    at = 0
    for piece in ins:
        all_ref[at : at + piece.shape[0], :] = piece[...]
        at += piece.shape[0]
    per = tok // KB
    for s in range(group):
        block = ((r ^ s) * rows) // QB
        for e in range(SEL):
            c = chosen_ref[block, e]
            owner = c // per
            start = (kv - owner) * tok + (c - owner * per) * KB
            outs[s][e * KB : (e + 1) * KB, :] = all_ref[pl.ds(pl.multiple_of(start, KB), KB), :]


def attend_kernel(where_ref, pos_ref, *refs, n, group, rows, heads):
    q_refs, kv_refs, out_ref = refs[:n], refs[n : n + group], refs[n + group]
    kv, t, r = where_ref[0], where_ref[1], where_ref[2]
    part = HD // group
    loaded = [ref[...] for ref in kv_refs]

    def column(j, lo):
        picked = loaded[0][:, lo : lo + part]
        for s in range(1, group):
            picked = jnp.where((r ^ s) == j, loaded[s][:, lo : lo + part], picked)
        return picked

    keys = jnp.concatenate([column(j, 0) for j in range(group)], axis=1)
    values = jnp.concatenate([column(j, part) for j in range(group)], axis=1)
    first = r * rows
    key_pos = pos_ref[first // QB]
    query_pos = kv * (group * rows) + first + lax.broadcasted_iota(jnp.int32, (rows, 1), 0)
    allowed = key_pos <= query_pos
    scale = 1.0 / math.sqrt(HD)
    for s in range(n):
        for m in range(heads):
            q = q_refs[s][:, m * HD : (m + 1) * HD]
            scores = lax.dot_general(
                q, keys, (((1,), (1,)), ((), ())), preferred_element_type=jnp.float32
            )
            scores = jnp.where(allowed, scores * scale, -jnp.inf)
            peak = jnp.max(scores, axis=1, keepdims=True)
            weight = jnp.exp(scores - peak)
            weight = (weight / jnp.sum(weight, axis=1, keepdims=True)).astype(jnp.bfloat16)
            result = jnp.dot(weight, values, preferred_element_type=jnp.float32)
            out_ref[(t ^ s) * heads + m] = result.astype(jnp.bfloat16)


def project_kernel(where_ref, gain_ref, weight_ref, *refs, group, rows, first, width):
    pieces = refs[:group]
    if first:
        sum_ref, energy_ref, gained_ref = refs[group:]
    else:
        prior_ref, prior_energy_ref, out_ref, gained_ref, energy_ref = refs[group:]
    r = where_ref[2]
    g = where_ref[3] if first else KVH - 1 - where_ref[3]
    blocks = pieces[0].shape[0]
    for s in range(group):
        row = pl.ds(pl.multiple_of((r ^ s) * rows, rows), rows)
        energy = jnp.zeros((rows, HD), jnp.float32)
        for m in range(blocks):
            x = pieces[s][m].astype(jnp.float32)
            energy += x * x
            gain = gain_ref[pl.ds(m * KVH + g, 1), :]
            gained_ref[row, m * HD : (m + 1) * HD] = (x * gain).astype(jnp.bfloat16)
        energy_ref[row, :] = energy
    columns = weight_ref.shape[-1]
    step = min(256, columns)
    if not first:
        total = jnp.sum(prior_energy_ref[...] + energy_ref[...], axis=1, keepdims=True)
        row_scale = lax.rsqrt(total / width + 1e-06)
    for lo in range(0, columns, step):
        cols = slice(lo, lo + step)
        acc = None
        for m in range(0, blocks, 2):
            w = jnp.concatenate([weight_ref[m, g, :, cols], weight_ref[m + 1, g, :, cols]], axis=0)
            d = jnp.dot(
                gained_ref[:, m * HD : (m + 2) * HD], w, preferred_element_type=jnp.float32
            )
            acc = d if acc is None else acc + d
        if first:
            sum_ref[:, cols] = acc
        else:
            out_ref[:, cols] = ((prior_ref[:, cols] + acc) * row_scale).astype(jnp.bfloat16)


def per_device(
    activations, query_weight, key_weight, value_weight, chosen, out_gain, out_weight, *, n_kv, n_tp
):
    tok = activations.shape[0]
    group = n_tp // KVH
    rows = tok // group
    heads = query_weight.shape[1] // HD // KVH
    blocks = chosen.shape[0]
    bf16, f32 = jnp.bfloat16, jnp.float32
    kv, t = lax.axis_index("kv"), lax.axis_index("tp")
    g, r = t // group, t % group
    where = jnp.stack([kv, t, r, g]).astype(jnp.int32)

    key_part = jnp.dot(activations, key_weight, preferred_element_type=f32).astype(bf16)
    value_part = jnp.dot(activations, value_weight, preferred_element_type=f32).astype(bf16)
    kv_part = jnp.concatenate([key_part, value_part], axis=1)
    pieces = gather_before(kv_part, n_kv)

    queries = jnp.dot(activations, query_weight, preferred_element_type=f32).astype(bf16)
    by_owner = queries.reshape(group, rows, heads, KVH, HD).transpose(3, 0, 1, 2, 4)
    by_owner = by_owner.reshape(n_tp, rows, heads * HD)
    q_pieces = [lax.dynamic_index_in_dim(by_owner, t ^ s, 0, False) for s in range(n_tp)]
    q_pieces = [q_pieces[0]] + [swap(q_pieces[s], n_tp, s) for s in range(1, n_tp)]

    offsets = jnp.arange(KB, dtype=jnp.int32)
    repeats = chosen[:, :, None] == chosen[:, None, :]
    preceding = jnp.arange(SEL)[None, :] < jnp.arange(SEL)[:, None]
    fresh = jnp.logical_not(jnp.any(repeats & preceding[None], axis=2))
    key_pos = jnp.where(fresh[:, :, None], chosen[:, :, None] * KB + offsets, FAR)
    key_pos = key_pos.reshape(blocks, 1, SEL * KB)

    width_kv = kv_part.shape[1]
    picked = pl.pallas_call(
        functools.partial(
            select_kernel, pieces=len(pieces), group=group, rows=rows, tok=tok
        ),
        out_shape=[jax.ShapeDtypeStruct((SEL * KB, width_kv), bf16)] * group,
        in_specs=[SMEM, SMEM] + [VMEM] * len(pieces),
        out_specs=[VMEM] * group,
        scratch_shapes=[pltpu.VMEM((n_kv * tok, width_kv), bf16)],
        name="select",
    )(where, chosen, *pieces)
    picked = [picked[0]] + [swap(picked[s], n_tp, s) for s in range(1, group)]

    attended = pl.pallas_call(
        functools.partial(attend_kernel, n=n_tp, group=group, rows=rows, heads=heads),
        out_shape=jax.ShapeDtypeStruct((n_tp * heads, rows, HD), bf16),
        in_specs=[SMEM, VMEM] + [VMEM] * (n_tp + group),
        out_specs=VMEM,
        name="attend",
    )(where, key_pos, *q_pieces, *picked)

    across = swap(attended, n_tp, group)
    same = [attended] + [swap(attended, n_tp, s) for s in range(1, group)]
    other = [across] + [swap(across, n_tp, s) for s in range(1, group)]

    width, columns = out_weight.shape
    all_blocks = n_tp * heads
    weight = out_weight.reshape(all_blocks, KVH, HD, columns)
    gain = out_gain.reshape(all_blocks * KVH, HD)
    project = functools.partial(project_kernel, group=group, rows=rows, width=width)
    gained_shape = pltpu.VMEM((tok, all_blocks * HD), bf16)
    partial_sum, energy = pl.pallas_call(
        functools.partial(project, first=True),
        out_shape=[
            jax.ShapeDtypeStruct((tok, columns), f32),
            jax.ShapeDtypeStruct((tok, HD), f32),
        ],
        in_specs=[SMEM] + [VMEM] * (2 + group),
        out_specs=[VMEM, VMEM],
        scratch_shapes=[gained_shape],
        name="project_same",
    )(where, gain, weight, *same)
    return pl.pallas_call(
        functools.partial(project, first=False),
        out_shape=jax.ShapeDtypeStruct((tok, columns), bf16),
        in_specs=[SMEM] + [VMEM] * (4 + group),
        out_specs=VMEM,
        scratch_shapes=[gained_shape, pltpu.VMEM((tok, HD), f32)],
        name="project_other",
    )(where, gain, weight, *other, partial_sum, energy)


def solution(mesh):
    in_specs = (
        P("kv", None),
        P(None, "tp"),
        P(None, "tp"),
        P(None, "tp"),
        P("kv", None),
        P(),
        P(None, "tp"),
    )
    out_specs = P("kv", "tp")
    return jax.shard_map(
        functools.partial(per_device, n_kv=mesh.shape["kv"], n_tp=mesh.shape["tp"]),
        mesh=mesh,
        in_specs=in_specs,
        out_specs=out_specs,
        check_vma=False,
    )
```

```python
import functools
import math

import jax
import jax.numpy as jnp
from jax import lax
from jax.experimental import pallas as pl
from jax.experimental.pallas import tpu as pltpu
from jax.sharding import PartitionSpec as P

HD = 128
KVH = 2
QB = 128
KB = 32
SEL = 16
FAR = 2**30


VMEM = pl.BlockSpec(memory_space=pltpu.VMEM)
SMEM = pl.BlockSpec(memory_space=pltpu.SMEM)


def in_vmem(x):
    return pltpu.with_memory_space_constraint(x, pltpu.VMEM) if x.size <= 2**19 else x


def call(kernel, outs, ins, scalars, scratch, name):
    ins = [in_vmem(x) for x in ins]
    return pl.pallas_call(
        kernel,
        out_shape=[pltpu.VMEM(shape, dtype) for shape, dtype in outs],
        in_specs=[SMEM] * len(scalars) + [VMEM] * len(ins),
        out_specs=[VMEM] * len(outs),
        scratch_shapes=scratch,
        name=name,
    )(*scalars, *ins)


def kv_kernel(act_ref, key_ref, value_ref, out_ref, acc_ref):
    step = pl.program_id(0)
    both = jnp.concatenate([key_ref[...], value_ref[...]], axis=0)
    d = lax.dot_general(
        act_ref[...], both, (((1,), (1,)), ((), ())), preferred_element_type=jnp.float32
    )

    @pl.when(step == 0)
    def _():
        acc_ref[...] = d

    @pl.when(step > 0)
    def _():
        acc_ref[...] += d

    @pl.when(step == pl.num_programs(0) - 1)
    def _():
        out_ref[...] = acc_ref[...].astype(jnp.bfloat16)


def project_kv(activations, key_weight, value_weight, steps=8):
    tok, depth = activations.shape
    cols = key_weight.shape[1]
    chunk = depth // steps
    return pl.pallas_call(
        kv_kernel,
        grid=(steps,),
        out_shape=pltpu.VMEM((tok, 2 * cols), jnp.bfloat16),
        in_specs=[
            pl.BlockSpec((tok, chunk), lambda i: (0, i)),
            pl.BlockSpec((cols, chunk), lambda i: (0, i)),
            pl.BlockSpec((cols, chunk), lambda i: (0, i)),
        ],
        out_specs=VMEM,
        scratch_shapes=[pltpu.VMEM((tok, 2 * cols), jnp.float32)],
        name="project_kv",
    )(activations, key_weight.T, value_weight.T)


def gather_before(part, n):
    half = n // 2
    if n > 16:
        every = lax.all_gather(part, "kv", axis=0, tiled=False)
        back = 2 * jnp.arange(half, dtype=jnp.int32)
        at = lax.axis_index("kv")
        near = jnp.take(every, (at - back) % n, axis=0).reshape(-1, part.shape[1])
        far = jnp.take(every, ((at ^ 1) - back) % n, axis=0).reshape(-1, part.shape[1])
        return [near, far]
    near = [part] + [
        lax.ppermute(part, "kv", [(i, (i + 2 * s) % n) for i in range(n)]) for s in range(1, half)
    ]
    near = jnp.concatenate(near, axis=0)
    return [near, lax.ppermute(near, "kv", [(i, i ^ 1) for i in range(n)])]


def swap(x, n, s):
    return lax.ppermute(x, "tp", [(i, i ^ s) for i in range(n)])


def select_kernel(where_ref, chosen_ref, *refs, pieces, group, rows, tok):
    ins, outs, all_ref = refs[:pieces], refs[pieces : pieces + group], refs[-1]
    kv, r = where_ref[0], where_ref[2]
    at = 0
    for piece in ins:
        all_ref[at : at + piece.shape[0], :] = piece[...]
        at += piece.shape[0]
    per = tok // KB
    for s in range(group):
        block = ((r ^ s) * rows) // QB
        for e in range(SEL):
            c = chosen_ref[block, e]
            owner = c // per
            away = (kv ^ owner) & 1
            back = ((kv ^ away) - owner) // 2
            start = (away * (at // 2 // tok) + back) * tok + (c - owner * per) * KB
            outs[s][e * KB : (e + 1) * KB, :] = all_ref[pl.ds(pl.multiple_of(start, KB), KB), :]


def attend_kernel(where_ref, pos_ref, *refs, n, group, rows, heads):
    q_refs, kv_refs, out_ref = refs[:n], refs[n : n + group], refs[n + group]
    kv, t, r = where_ref[0], where_ref[1], where_ref[2]
    part = HD // group
    loaded = [ref[...] for ref in kv_refs]

    def column(j, lo):
        picked = loaded[0][:, lo : lo + part]
        for s in range(1, group):
            picked = jnp.where((r ^ s) == j, loaded[s][:, lo : lo + part], picked)
        return picked

    keys = jnp.concatenate([column(j, 0) for j in range(group)], axis=1)
    values = jnp.concatenate([column(j, part) for j in range(group)], axis=1)
    first = r * rows
    key_pos = pos_ref[first // QB]
    query_pos = kv * (group * rows) + first + lax.broadcasted_iota(jnp.int32, (rows, 1), 0)
    allowed = key_pos <= query_pos
    scale = math.log2(math.e) / math.sqrt(HD)
    for s in range(n):
        for m in range(heads):
            q = q_refs[s][:, m * HD : (m + 1) * HD]
            scores = lax.dot_general(
                q, keys, (((1,), (1,)), ((), ())), preferred_element_type=jnp.float32
            )
            scores = jnp.where(allowed, scores, -jnp.inf)
            peak = jnp.max(scores, axis=1, keepdims=True)
            weight = jnp.exp2((scores - peak) * scale)
            weight = (weight * (1.0 / jnp.sum(weight, axis=1, keepdims=True))).astype(jnp.bfloat16)
            result = jnp.dot(weight, values, preferred_element_type=jnp.float32)
            out_ref[(t ^ s) * heads + m] = result.astype(jnp.bfloat16)


def project_kernel(where_ref, gain_ref, weight_ref, *refs, group, rows, first, width):
    pieces = refs[:group]
    if first:
        sum_ref, energy_ref, gained_ref = refs[group:]
    else:
        prior_ref, prior_energy_ref, out_ref, gained_ref, energy_ref = refs[group:]
    r = where_ref[2]
    g = where_ref[3] if first else KVH - 1 - where_ref[3]
    blocks = pieces[0].shape[0]
    step = pl.program_id(0)

    @pl.when(step == 0)
    def _():
        for s in range(group):
            row = pl.ds(pl.multiple_of((r ^ s) * rows, rows), rows)
            energy = jnp.zeros((rows, HD), jnp.float32)
            for m in range(blocks):
                x = pieces[s][m].astype(jnp.float32)
                energy += x * x
                gain = gain_ref[pl.ds(m * KVH + g, 1), :]
                gained_ref[row, m * HD : (m + 1) * HD] = (x * gain).astype(jnp.bfloat16)
            energy_ref[row, :] = energy

    w = weight_ref[...].reshape(blocks * HD, weight_ref.shape[-1])
    acc = jnp.dot(gained_ref[...], w, preferred_element_type=jnp.float32)
    if first:
        sum_ref[...] = acc
    else:
        total = jnp.sum(prior_energy_ref[...] + energy_ref[...], axis=1, keepdims=True)
        row_scale = lax.rsqrt(total / width + 1e-06)
        out_ref[...] = ((prior_ref[...] + acc) * row_scale).astype(jnp.bfloat16)


def project(where, gain, weight, pieces, prior, width, group, rows):
    first = prior is None
    blocks, _, _, columns = weight.shape
    tok = group * rows
    wide = min(256, columns)
    kernel = functools.partial(
        project_kernel, group=group, rows=rows, first=first, width=width
    )
    pieces = [in_vmem(x) for x in pieces]
    weight_spec = pl.BlockSpec(
        (blocks, None, HD, wide),
        (lambda i, at: (0, at[3], 0, i)) if first else (lambda i, at: (0, KVH - 1 - at[3], 0, i)),
    )
    tile = pl.BlockSpec((tok, wide), lambda i, at: (0, i))
    scratch = [pltpu.VMEM((tok, blocks * HD), jnp.bfloat16)]
    f32 = jnp.float32
    if first:
        outs = [jax.ShapeDtypeStruct((tok, columns), f32), pltpu.VMEM((tok, HD), f32)]
        in_specs, out_specs, ins = [], [tile, VMEM], pieces
    else:
        outs, out_specs = jax.ShapeDtypeStruct((tok, columns), jnp.bfloat16), tile
        scratch += [pltpu.VMEM((tok, HD), f32)]
        total, energy = prior
        in_specs = [tile, VMEM]
        ins = [*pieces, total, in_vmem(energy)]
    return pl.pallas_call(
        kernel,
        grid_spec=pltpu.PrefetchScalarGridSpec(
            num_scalar_prefetch=1,
            grid=(columns // wide,),
            in_specs=[VMEM, weight_spec] + [VMEM] * group + in_specs,
            out_specs=out_specs,
            scratch_shapes=scratch,
        ),
        out_shape=outs,
        cost_estimate=pl.CostEstimate(
            flops=2 * tok * blocks * HD * columns,
            bytes_accessed=2 * blocks * HD * columns,
            transcendentals=0,
        ),
        name="project_same" if first else "project_other",
    )(where, gain, weight, *ins)


def per_device(
    activations, query_weight, key_weight, value_weight, chosen, out_gain, out_weight, *, n_kv, n_tp
):
    tok = activations.shape[0]
    group = n_tp // KVH
    rows = tok // group
    heads = query_weight.shape[1] // HD // KVH
    blocks = chosen.shape[0]
    bf16, f32 = jnp.bfloat16, jnp.float32
    kv, t = lax.axis_index("kv"), lax.axis_index("tp")
    g, r = t // group, t % group
    where = jnp.stack([kv, t, r, g]).astype(jnp.int32)

    kv_part = project_kv(activations, key_weight, value_weight)
    pieces = gather_before(kv_part, n_kv)

    queries = jnp.dot(activations, query_weight, preferred_element_type=f32).astype(bf16)
    by_owner = queries.reshape(group, rows, heads, KVH, HD).transpose(3, 0, 1, 2, 4)
    by_owner = by_owner.reshape(n_tp, rows, heads * HD)
    q_pieces = [lax.dynamic_index_in_dim(by_owner, t ^ s, 0, False) for s in range(n_tp)]
    q_pieces = [q_pieces[0]] + [swap(q_pieces[s], n_tp, s) for s in range(1, n_tp)]

    offsets = jnp.arange(KB, dtype=jnp.int32)
    repeats = chosen[:, :, None] == chosen[:, None, :]
    preceding = jnp.arange(SEL)[None, :] < jnp.arange(SEL)[:, None]
    fresh = jnp.logical_not(jnp.any(repeats & preceding[None], axis=2))
    key_pos = jnp.where(fresh[:, :, None], chosen[:, :, None] * KB + offsets, FAR)
    key_pos = key_pos.reshape(blocks, 1, SEL * KB)

    width_kv = kv_part.shape[1]
    picked = call(
        functools.partial(select_kernel, pieces=len(pieces), group=group, rows=rows, tok=tok),
        [((SEL * KB, width_kv), bf16)] * group,
        pieces,
        [where, chosen],
        [pltpu.VMEM((n_kv * tok, width_kv), bf16)],
        "select",
    )
    picked = [picked[0]] + [swap(picked[s], n_tp, s) for s in range(1, group)]

    all_blocks = n_tp * heads
    (attended,) = call(
        functools.partial(attend_kernel, n=n_tp, group=group, rows=rows, heads=heads),
        [((all_blocks, rows, HD), bf16)],
        [key_pos, *q_pieces, *picked],
        [where],
        [],
        "attend",
    )

    across = swap(attended, n_tp, group)
    same = [attended] + [swap(attended, n_tp, s) for s in range(1, group)]

    width, columns = out_weight.shape
    weight = out_weight.reshape(all_blocks, KVH, HD, columns)
    gain = out_gain.reshape(all_blocks * KVH, HD)
    partial_sum, energy = project(where, gain, weight, same, None, width, group, rows)
    across, energy = lax.optimization_barrier((across, energy))
    other = [across] + [swap(across, n_tp, s) for s in range(1, group)]
    return project(where, gain, weight, other, (partial_sum, energy), width, group, rows)


def solution(mesh):
    in_specs = (
        P("kv", None),
        P(None, "tp"),
        P(None, "tp"),
        P(None, "tp"),
        P("kv", None),
        P(),
        P(None, "tp"),
    )
    out_specs = P("kv", "tp")
    return jax.shard_map(
        functools.partial(per_device, n_kv=mesh.shape["kv"], n_tp=mesh.shape["tp"]),
        mesh=mesh,
        in_specs=in_specs,
        out_specs=out_specs,
        check_vma=False,
    )
```

```python
import functools
import math

import jax
import jax.numpy as jnp
from jax import lax
from jax.experimental import pallas as pl
from jax.experimental.pallas import tpu as pltpu
from jax.sharding import PartitionSpec as P

HD = 128
KVH = 2
QB = 128
KB = 32
SEL = 16
FAR = 2**30


VMEM = pl.BlockSpec(memory_space=pltpu.VMEM)
SMEM = pl.BlockSpec(memory_space=pltpu.SMEM)
ANY = pl.BlockSpec(memory_space=pltpu.HBM)


def in_vmem(x):
    return pltpu.with_memory_space_constraint(x, pltpu.VMEM) if x.size <= 2**19 else x


def call(kernel, outs, ins, scalars, scratch, name):
    ins = [in_vmem(x) for x in ins]
    return pl.pallas_call(
        kernel,
        out_shape=[pltpu.VMEM(shape, dtype) for shape, dtype in outs],
        in_specs=[SMEM] * len(scalars) + [VMEM] * len(ins),
        out_specs=[VMEM] * len(outs),
        scratch_shapes=scratch,
        name=name,
    )(*scalars, *ins)


def kv_kernel(act_hbm, key_hbm, value_hbm, out_ref, act_ref, both_ref, sems, *, chunk):
    tok, cols = act_ref.shape[0], key_hbm.shape[0]
    copies = [
        pltpu.make_async_copy(key_hbm, both_ref.at[0:cols], sems.at[0]),
        pltpu.make_async_copy(value_hbm, both_ref.at[cols : 2 * cols], sems.at[1]),
    ]
    for i in range(tok // chunk):
        rows = slice(i * chunk, (i + 1) * chunk)
        copies.append(pltpu.make_async_copy(act_hbm.at[rows], act_ref.at[rows], sems.at[2 + i]))
    for copy in copies:
        copy.start()
    copies[0].wait()
    copies[1].wait()
    for i in range(tok // chunk):
        rows = slice(i * chunk, (i + 1) * chunk)
        copies[2 + i].wait()
        out_ref[rows, :] = lax.dot_general(
            act_ref[rows, :],
            both_ref[...],
            (((1,), (1,)), ((), ())),
            preferred_element_type=jnp.float32,
        ).astype(jnp.bfloat16)


def project_kv(activations, key_weight, value_weight, chunk=64):
    tok, depth = activations.shape
    cols = key_weight.shape[1]
    bf16 = jnp.bfloat16
    return pl.pallas_call(
        functools.partial(kv_kernel, chunk=chunk),
        out_shape=[pltpu.VMEM((tok, 2 * cols), bf16), pltpu.VMEM((tok, depth), bf16)],
        in_specs=[ANY] * 3,
        out_specs=[VMEM, VMEM],
        scratch_shapes=[
            pltpu.VMEM((2 * cols, depth), bf16),
            pltpu.SemaphoreType.DMA((2 + tok // chunk,)),
        ],
        name="project_kv",
    )(activations, key_weight.T, value_weight.T)


def gather_before(part, queries, n):
    half = n // 2
    if n > 16:
        every = lax.all_gather(part, "kv", axis=0, tiled=False)
        back = 2 * jnp.arange(half, dtype=jnp.int32)
        at = lax.axis_index("kv")
        near = jnp.take(every, (at - back) % n, axis=0).reshape(-1, part.shape[1])
        far = jnp.take(every, ((at ^ 1) - back) % n, axis=0).reshape(-1, part.shape[1])
        return [near, far], queries
    near = [part] + [
        lax.ppermute(part, "kv", [(i, (i + 2 * s) % n) for i in range(n)]) for s in range(1, half)
    ]
    near = jnp.concatenate(near, axis=0)
    near, queries = lax.optimization_barrier((near, queries))
    return [near, lax.ppermute(near, "kv", [(i, i ^ 1) for i in range(n)])], queries


def swap(x, n, s):
    return lax.ppermute(x, "tp", [(i, i ^ s) for i in range(n)])


def select_kernel(where_ref, chosen_ref, *refs, pieces, group, rows, tok):
    ins, outs, all_ref = refs[:pieces], refs[pieces : pieces + group], refs[-1]
    kv, r = where_ref[0], where_ref[2]
    at = 0
    for piece in ins:
        all_ref[at : at + piece.shape[0], :] = piece[...]
        at += piece.shape[0]
    per = tok // KB
    for s in range(group):
        block = ((r ^ s) * rows) // QB
        for e in range(SEL):
            c = chosen_ref[block, e]
            owner = c // per
            away = (kv ^ owner) & 1
            back = ((kv ^ away) - owner) // 2
            start = (away * (at // 2 // tok) + back) * tok + (c - owner * per) * KB
            outs[s][e * KB : (e + 1) * KB, :] = all_ref[pl.ds(pl.multiple_of(start, KB), KB), :]


def attend_kernel(where_ref, pos_ref, *refs, n, group, rows, heads):
    q_refs, kv_refs, out_ref = refs[:n], refs[n : n + group], refs[n + group]
    kv, t, r = where_ref[0], where_ref[1], where_ref[2]
    part = HD // group
    loaded = [ref[...] for ref in kv_refs]

    def column(j, lo):
        picked = loaded[0][:, lo : lo + part]
        for s in range(1, group):
            picked = jnp.where((r ^ s) == j, loaded[s][:, lo : lo + part], picked)
        return picked

    keys = jnp.concatenate([column(j, 0) for j in range(group)], axis=1)
    values = jnp.concatenate([column(j, part) for j in range(group)], axis=1)
    first = r * rows
    key_pos = pos_ref[first // QB]
    query_pos = kv * (group * rows) + first + lax.broadcasted_iota(jnp.int32, (rows, 1), 0)
    allowed = key_pos <= query_pos
    scale = math.log2(math.e) / math.sqrt(HD)
    for s in range(n):
        for m in range(heads):
            q = q_refs[s][:, m * HD : (m + 1) * HD]
            scores = lax.dot_general(
                q, keys, (((1,), (1,)), ((), ())), preferred_element_type=jnp.float32
            )
            scores = jnp.where(allowed, scores, -jnp.inf)
            peak = jnp.max(scores, axis=1, keepdims=True)
            weight = jnp.exp2((scores - peak) * scale)
            weight = (weight * (1.0 / jnp.sum(weight, axis=1, keepdims=True))).astype(jnp.bfloat16)
            result = jnp.dot(weight, values, preferred_element_type=jnp.float32)
            out_ref[(t ^ s) * heads + m] = result.astype(jnp.bfloat16)


def gain_pieces(pieces, gain_ref, gained_ref, energy_ref, r, g, rows):
    for s, piece in enumerate(pieces):
        row = pl.ds(pl.multiple_of((r ^ s) * rows, rows), rows)
        energy = jnp.zeros((rows, HD), jnp.float32)
        for m in range(piece.shape[0]):
            x = piece[m].astype(jnp.float32)
            energy += x * x
            gain = gain_ref[pl.ds(m * KVH + g, 1), :]
            gained_ref[row, m * HD : (m + 1) * HD] = (x * gain).astype(jnp.bfloat16)
        energy_ref[row, :] = energy


def weight_copies(weight_hbm, now_ref, sems, g):
    copies = []
    for m in range(weight_hbm.shape[0]):
        at = slice(m * HD, (m + 1) * HD)
        copies.append(pltpu.make_async_copy(weight_hbm.at[m, g], now_ref.at[at], sems.at[m]))
    return copies


def product(gained_ref, now_ref, copies, parts=2):
    acc, share = None, len(copies) // parts
    for i in range(parts):
        for copy in copies[i * share : (i + 1) * share]:
            copy.wait()
        at = slice(i * share * HD, (i + 1) * share * HD)
        d = jnp.dot(gained_ref[:, at], now_ref[at, :], preferred_element_type=jnp.float32)
        acc = d if acc is None else acc + d
    return acc


def same_kernel(where_ref, gain_ref, weight_hbm, *refs, group, rows):
    pieces = refs[:group]
    sum_ref, energy_ref, gained_ref, now_ref, sems = refs[group:]
    r, g = where_ref[2], where_ref[3]
    copies = weight_copies(weight_hbm, now_ref, sems, g)
    for copy in copies:
        copy.start()
    gain_pieces(pieces, gain_ref, gained_ref, energy_ref, r, g, rows)
    sum_ref[...] = product(gained_ref, now_ref, copies)


def other_kernel(where_ref, gain_ref, weight_hbm, *refs, group, rows, width):
    pieces = refs[:group]
    prior_ref, prior_energy_ref, out_ref, gained_ref, energy_ref, now_ref, sems = refs[group:]
    r, g = where_ref[2], KVH - 1 - where_ref[3]
    copies = weight_copies(weight_hbm, now_ref, sems, g)
    for copy in copies:
        copy.start()
    gain_pieces(pieces, gain_ref, gained_ref, energy_ref, r, g, rows)
    total = jnp.sum(prior_energy_ref[...] + energy_ref[...], axis=1, keepdims=True)
    row_scale = lax.rsqrt(total / width + 1e-06)
    acc = product(gained_ref, now_ref, copies)
    out_ref[...] = ((prior_ref[...] + acc) * row_scale).astype(jnp.bfloat16)


def per_device(
    activations, query_weight, key_weight, value_weight, chosen, out_gain, out_weight, *, n_kv, n_tp
):
    tok = activations.shape[0]
    group = n_tp // KVH
    rows = tok // group
    heads = query_weight.shape[1] // HD // KVH
    blocks = chosen.shape[0]
    bf16, f32 = jnp.bfloat16, jnp.float32
    kv, t = lax.axis_index("kv"), lax.axis_index("tp")
    g, r = t // group, t % group
    where = jnp.stack([kv, t, r, g]).astype(jnp.int32)

    kv_part, act_near = project_kv(activations, key_weight, value_weight)
    queries = jnp.dot(act_near, query_weight, preferred_element_type=f32).astype(bf16)
    pieces, queries = gather_before(kv_part, queries, n_kv)
    by_owner = queries.reshape(group, rows, heads, KVH, HD).transpose(3, 0, 1, 2, 4)
    by_owner = by_owner.reshape(n_tp, rows, heads * HD)
    q_pieces = [lax.dynamic_index_in_dim(by_owner, t ^ s, 0, False) for s in range(n_tp)]
    q_pieces = [q_pieces[0]] + [swap(q_pieces[s], n_tp, s) for s in range(1, n_tp)]

    offsets = jnp.arange(KB, dtype=jnp.int32)
    repeats = chosen[:, :, None] == chosen[:, None, :]
    preceding = jnp.arange(SEL)[None, :] < jnp.arange(SEL)[:, None]
    fresh = jnp.logical_not(jnp.any(repeats & preceding[None], axis=2))
    key_pos = jnp.where(fresh[:, :, None], chosen[:, :, None] * KB + offsets, FAR)
    key_pos = key_pos.reshape(blocks, 1, SEL * KB)

    width_kv = kv_part.shape[1]
    picked = call(
        functools.partial(select_kernel, pieces=len(pieces), group=group, rows=rows, tok=tok),
        [((SEL * KB, width_kv), bf16)] * group,
        pieces,
        [where, chosen],
        [pltpu.VMEM((n_kv * tok, width_kv), bf16)],
        "select",
    )
    picked = [picked[0]] + [swap(picked[s], n_tp, s) for s in range(1, group)]

    all_blocks = n_tp * heads
    (attended,) = call(
        functools.partial(attend_kernel, n=n_tp, group=group, rows=rows, heads=heads),
        [((all_blocks, rows, HD), bf16)],
        [key_pos, *q_pieces, *picked],
        [where],
        [],
        "attend",
    )

    across = swap(attended, n_tp, group)
    same = [attended] + [swap(attended, n_tp, s) for s in range(1, group)]

    width, columns = out_weight.shape
    weight = out_weight.reshape(all_blocks, KVH, HD, columns)
    gain = out_gain.reshape(all_blocks * KVH, HD)
    scratch = [
        pltpu.VMEM((tok, all_blocks * HD), bf16),
        pltpu.VMEM((all_blocks * HD, columns), bf16),
        pltpu.SemaphoreType.DMA((all_blocks,)),
    ]
    partial_sum, energy = pl.pallas_call(
        functools.partial(same_kernel, group=group, rows=rows),
        out_shape=[pltpu.VMEM((tok, columns), f32), pltpu.VMEM((tok, HD), f32)],
        in_specs=[SMEM, VMEM, ANY] + [VMEM] * group,
        out_specs=[VMEM] * 2,
        scratch_shapes=scratch,
        name="project_same",
    )(where, gain, weight, *[in_vmem(x) for x in same])
    across, energy = lax.optimization_barrier((across, energy))
    other = [across] + [swap(across, n_tp, s) for s in range(1, group)]
    return pl.pallas_call(
        functools.partial(other_kernel, group=group, rows=rows, width=width),
        out_shape=jax.ShapeDtypeStruct((tok, columns), bf16),
        in_specs=[SMEM, VMEM, ANY] + [VMEM] * (group + 2),
        out_specs=VMEM,
        scratch_shapes=[scratch[0], pltpu.VMEM((tok, HD), f32), *scratch[1:]],
        name="project_other",
    )(where, gain, weight, *[in_vmem(x) for x in [*other, partial_sum, energy]])


def solution(mesh):
    in_specs = (
        P("kv", None),
        P(None, "tp"),
        P(None, "tp"),
        P(None, "tp"),
        P("kv", None),
        P(),
        P(None, "tp"),
    )
    out_specs = P("kv", "tp")
    return jax.shard_map(
        functools.partial(per_device, n_kv=mesh.shape["kv"], n_tp=mesh.shape["tp"]),
        mesh=mesh,
        in_specs=in_specs,
        out_specs=out_specs,
        check_vma=False,
    )
```

```python
import functools
import math

import jax
import jax.numpy as jnp
from jax import lax
from jax.experimental import pallas as pl
from jax.experimental.pallas import tpu as pltpu
from jax.sharding import PartitionSpec as P


HD = 128
KVH = 2
QB = 128
KB = 32
SEL = 16
FAR = 2**30


VMEM = pl.BlockSpec(memory_space=pltpu.VMEM)
SMEM = pl.BlockSpec(memory_space=pltpu.SMEM)
ANY = pl.BlockSpec(memory_space=pltpu.HBM)


def in_vmem(x):
    return pltpu.with_memory_space_constraint(x, pltpu.VMEM) if x.size <= 2**19 else x


def call(kernel, outs, ins, scalars, scratch, flops=0):
    ins = [in_vmem(x) for x in ins]
    return pl.pallas_call(
        kernel,
        out_shape=[pltpu.VMEM(shape, dtype) for shape, dtype in outs],
        in_specs=[SMEM] * len(scalars) + [VMEM] * len(ins),
        out_specs=[VMEM] * len(outs),
        scratch_shapes=scratch,
        cost_estimate=pl.CostEstimate(flops=flops, bytes_accessed=0, transcendentals=0),
    )(*scalars, *ins)


def kv_kernel(act_hbm, key_hbm, value_hbm, out_ref, act_ref, both_ref, sems, *, chunk):
    tok, cols = act_ref.shape[0], key_hbm.shape[0]
    copies = [
        pltpu.make_async_copy(key_hbm, both_ref.at[0:cols], sems.at[0]),
        pltpu.make_async_copy(value_hbm, both_ref.at[cols : 2 * cols], sems.at[1]),
    ]
    for i in range(tok // chunk):
        rows = slice(i * chunk, (i + 1) * chunk)
        copies.append(pltpu.make_async_copy(act_hbm.at[rows], act_ref.at[rows], sems.at[2 + i]))
    for copy in copies:
        copy.start()
    copies[0].wait()
    copies[1].wait()
    for i in range(tok // chunk):
        rows = slice(i * chunk, (i + 1) * chunk)
        copies[2 + i].wait()
        out_ref[rows, :] = lax.dot_general(
            act_ref[rows, :],
            both_ref[...],
            (((1,), (1,)), ((), ())),
            preferred_element_type=jnp.float32,
        ).astype(jnp.bfloat16)


def project_kv(activations, key_weight, value_weight, chunk=128):
    tok, depth = activations.shape
    cols = key_weight.shape[1]
    bf16 = jnp.bfloat16
    return pl.pallas_call(
        functools.partial(kv_kernel, chunk=chunk),
        out_shape=[pltpu.VMEM((tok, 2 * cols), bf16), pltpu.VMEM((tok, depth), bf16)],
        in_specs=[ANY] * 3,
        out_specs=[VMEM, VMEM],
        scratch_shapes=[
            pltpu.VMEM((2 * cols, depth), bf16),
            pltpu.SemaphoreType.DMA((2 + tok // chunk,)),
        ],
        name="project_kv",
    )(activations, key_weight.T, value_weight.T)


def gather_before(part, queries, n):
    half = n // 2
    if n > 16:
        every = lax.all_gather(part, "kv", axis=0, tiled=False)
        back = 2 * jnp.arange(half, dtype=jnp.int32)
        at = lax.axis_index("kv")
        near = jnp.take(every, (at - back) % n, axis=0).reshape(-1, part.shape[1])
        far = jnp.take(every, ((at ^ 1) - back) % n, axis=0).reshape(-1, part.shape[1])
        return [near, far], queries
    near = [part] + [
        lax.ppermute(part, "kv", [(i, (i + 2 * s) % n) for i in range(n)]) for s in range(1, half)
    ]
    near = jnp.concatenate(near, axis=0)
    near, queries = lax.optimization_barrier((near, queries))
    return [near, lax.ppermute(near, "kv", [(i, i ^ 1) for i in range(n)])], queries


def swap(x, n, s):
    return lax.ppermute(x, "tp", [(i, i ^ s) for i in range(n)])


def select_kernel(where_ref, chosen_ref, *refs, pieces, group, rows, tok):
    ins, outs, all_ref = refs[:pieces], refs[pieces : pieces + group], refs[-1]
    kv, r = where_ref[0], where_ref[2]
    at = 0
    for piece in ins:
        all_ref[at : at + piece.shape[0], :] = piece[...]
        at += piece.shape[0]
    per = tok // KB
    for s in range(group):
        block = ((r ^ s) * rows) // QB
        for e in range(SEL):
            c = chosen_ref[block, e]
            owner = c // per
            away = (kv ^ owner) & 1
            back = ((kv ^ away) - owner) // 2
            start = (away * (at // 2 // tok) + back) * tok + (c - owner * per) * KB
            outs[s][e * KB : (e + 1) * KB, :] = all_ref[pl.ds(pl.multiple_of(start, KB), KB), :]


def attend_kernel(where_ref, base_ref, *refs, sources, group, rows, heads):
    q_refs, kv_refs = refs[: len(sources)], refs[len(sources) : len(sources) + group]
    out_ref = refs[-1]
    kv, t, r = where_ref[0], where_ref[1], where_ref[2]
    part = HD // group
    loaded = [ref[...] for ref in kv_refs]

    def column(j, lo):
        picked = loaded[0][:, lo : lo + part]
        for s in range(1, group):
            picked = jnp.where((r ^ s) == j, loaded[s][:, lo : lo + part], picked)
        return picked

    keys = jnp.concatenate([column(j, 0) for j in range(group)], axis=1)
    values = jnp.concatenate([column(j, part) for j in range(group)], axis=1)
    values = values.astype(jnp.float32).T.astype(jnp.bfloat16)
    first = r * rows
    block = first // QB
    query_pos = kv * (group * rows) + first + lax.broadcasted_iota(jnp.int32, (KB, rows), 1)
    ahead = query_pos - lax.broadcasted_iota(jnp.int32, (KB, rows), 0)
    bias = [jnp.where(base_ref[block, e] <= ahead, 0.0, -jnp.inf) for e in range(SEL)]
    bias = jnp.concatenate(bias, axis=0)
    scale = math.log2(math.e) / math.sqrt(HD)
    for i, s in enumerate(sources):
        for m in range(heads):
            q = q_refs[i][:, m * HD : (m + 1) * HD]
            scores = bias + lax.dot_general(
                keys, q, (((1,), (1,)), ((), ())), preferred_element_type=jnp.float32
            )
            peak = jnp.max(scores, axis=0, keepdims=True)
            weight = jnp.exp2((scores - peak) * scale)
            weight = (weight * (1.0 / jnp.sum(weight, axis=0, keepdims=True))).astype(jnp.bfloat16)
            result = jnp.dot(values, weight, preferred_element_type=jnp.float32)
            out_ref[((t ^ s) % group) * heads + m] = result.T.astype(jnp.bfloat16)


def gain_pieces(pieces, gain_ref, gained_ref, energy_ref, r, g, starts, rows):
    count = pieces[0][0].shape[0]
    for s in range(len(pieces[0])):
        row = pl.ds(pl.multiple_of((r ^ s) * rows, rows), rows)
        energy = jnp.zeros((rows, HD), jnp.float32)
        for k, piece in enumerate(pieces):
            for m in range(count):
                x = piece[s][m].astype(jnp.float32)
                energy += x * x
                gain = gain_ref[pl.ds((starts[k] + m) * KVH + g, 1), :]
                at = (k * count + m) * HD
                gained_ref[row, at : at + HD] = (x * gain).astype(jnp.bfloat16)
        energy_ref[row, :] = energy


def weight_copies(weight_hbm, now_ref, sems, g, starts, count):
    copies = []
    for k, start in enumerate(starts):
        for m in range(count):
            i = k * count + m
            at = slice(i * HD, (i + 1) * HD)
            copies.append(
                pltpu.make_async_copy(weight_hbm.at[start + m, g], now_ref.at[at], sems.at[i])
            )
    return copies


def product(gained_ref, now_ref, copies, parts=2):
    acc, share = None, len(copies) // parts
    for i in range(parts):
        for copy in copies[i * share : (i + 1) * share]:
            copy.wait()
        at = slice(i * share * HD, (i + 1) * share * HD)
        d = jnp.dot(gained_ref[:, at], now_ref[at, :], preferred_element_type=jnp.float32)
        acc = d if acc is None else acc + d
    return acc


def same_kernel(where_ref, gain_ref, weight_hbm, *refs, group, rows):
    pieces = [refs[k * group : (k + 1) * group] for k in range(KVH)]
    sum_ref, energy_ref, gained_ref, now_ref, sems = refs[KVH * group :]
    r, g = where_ref[2], where_ref[3]
    count = weight_hbm.shape[0] // KVH
    starts = [(g ^ k) * count for k in range(KVH)]
    copies = weight_copies(weight_hbm, now_ref, sems, g, starts, count)
    for copy in copies:
        copy.start()
    gain_pieces(pieces, gain_ref, gained_ref, energy_ref, r, g, starts, rows)
    sum_ref[...] = product(gained_ref, now_ref, copies)


def other_kernel(where_ref, gain_ref, weight_hbm, *refs, group, rows, width):
    pieces = [refs[k * group : (k + 1) * group] for k in range(KVH)]
    prior_ref, prior_energy_ref, out_ref, gained_ref, energy_ref, now_ref, sems = refs[KVH * group :]
    r, g = where_ref[2], KVH - 1 - where_ref[3]
    count = weight_hbm.shape[0] // KVH
    starts = [(g ^ k) * count for k in range(KVH)]
    copies = weight_copies(weight_hbm, now_ref, sems, g, starts, count)
    for copy in copies:
        copy.start()
    gain_pieces(pieces, gain_ref, gained_ref, energy_ref, r, g, starts, rows)
    total = jnp.sum(prior_energy_ref[...] + energy_ref[...], axis=1, keepdims=True)
    row_scale = lax.rsqrt(total / width + 1e-06)
    acc = product(gained_ref, now_ref, copies)
    out_ref[...] = ((prior_ref[...] + acc) * row_scale).astype(jnp.bfloat16)


def per_device(
    activations, query_weight, key_weight, value_weight, chosen, out_gain, out_weight, *, n_kv, n_tp
):
    tok = activations.shape[0]
    group = n_tp // KVH
    rows = tok // group
    heads = query_weight.shape[1] // HD // KVH
    bf16, f32 = jnp.bfloat16, jnp.float32
    kv, t = lax.axis_index("kv"), lax.axis_index("tp")
    g, r = t // group, t % group
    where = jnp.stack([kv, t, r, g]).astype(jnp.int32)

    kv_part, act_near = project_kv(activations, key_weight, value_weight)
    queries = jnp.dot(act_near, query_weight, preferred_element_type=f32).astype(bf16)
    pieces, queries = gather_before(kv_part, queries, n_kv)
    by_owner = queries.reshape(group, rows, heads, KVH, HD).transpose(3, 0, 1, 2, 4)
    by_owner = by_owner.reshape(n_tp, rows, heads * HD)
    q_pieces = [lax.dynamic_index_in_dim(by_owner, t ^ s, 0, False) for s in range(n_tp)]
    q_pieces = [q_pieces[0]] + [swap(q_pieces[s], n_tp, s) for s in range(1, n_tp)]

    repeats = chosen[:, :, None] == chosen[:, None, :]
    preceding = jnp.arange(SEL)[None, :] < jnp.arange(SEL)[:, None]
    fresh = jnp.logical_not(jnp.any(repeats & preceding[None], axis=2))
    key_base = jnp.where(fresh, chosen * KB, FAR)

    width_kv = kv_part.shape[1]
    picked = call(
        functools.partial(select_kernel, pieces=len(pieces), group=group, rows=rows, tok=tok),
        [((SEL * KB, width_kv), bf16)] * group,
        pieces,
        [where, chosen],
        [pltpu.VMEM((n_kv * tok, width_kv), bf16)],
    )
    picked = [picked[0]] + [swap(picked[s], n_tp, s) for s in range(1, group)]

    all_blocks = n_tp * heads
    same, across = [], []
    for k in range(KVH):
        sources = [k * group + s for s in range(group)]
        (attended,) = call(
            functools.partial(
                attend_kernel, sources=sources, group=group, rows=rows, heads=heads
            ),
            [((group * heads, rows, HD), bf16)],
            [*[q_pieces[s] for s in sources], *picked],
            [where, key_base],
            [],
            flops=4 * SEL * KB * HD * rows * group * heads,
        )
        across.append(swap(attended, n_tp, group))
        same += [attended] + [swap(attended, n_tp, s) for s in range(1, group)]

    width, columns = out_weight.shape
    weight = out_weight.reshape(all_blocks, KVH, HD, columns)
    gain = out_gain.reshape(all_blocks * KVH, HD)
    scratch = [
        pltpu.VMEM((tok, all_blocks * HD), bf16),
        pltpu.VMEM((all_blocks * HD, columns), bf16),
        pltpu.SemaphoreType.DMA((all_blocks,)),
    ]
    partial_sum, energy = pl.pallas_call(
        functools.partial(same_kernel, group=group, rows=rows),
        out_shape=[pltpu.VMEM((tok, columns), f32), pltpu.VMEM((tok, HD), f32)],
        in_specs=[SMEM, VMEM, ANY] + [VMEM] * len(same),
        out_specs=[VMEM] * 2,
        scratch_shapes=scratch,
        name="project_same",
    )(where, gain, weight, *[in_vmem(x) for x in same])
    other = []
    for k in range(KVH):
        piece, energy = lax.optimization_barrier((across[k], energy))
        other += [piece] + [swap(piece, n_tp, s) for s in range(1, group)]
    return pl.pallas_call(
        functools.partial(other_kernel, group=group, rows=rows, width=width),
        out_shape=jax.ShapeDtypeStruct((tok, columns), bf16),
        in_specs=[SMEM, VMEM, ANY] + [VMEM] * (len(other) + 2),
        out_specs=VMEM,
        scratch_shapes=[scratch[0], pltpu.VMEM((tok, HD), f32), *scratch[1:]],
        name="project_other",
    )(where, gain, weight, *[in_vmem(x) for x in [*other, partial_sum, energy]])


def solution(mesh):
    in_specs = (
        P("kv", None),
        P(None, "tp"),
        P(None, "tp"),
        P(None, "tp"),
        P("kv", None),
        P(),
        P(None, "tp"),
    )
    out_specs = P("kv", "tp")
    body = functools.partial(per_device, n_kv=mesh.shape["kv"], n_tp=mesh.shape["tp"])

    return jax.shard_map(body, mesh=mesh, in_specs=in_specs, out_specs=out_specs, check_vma=False)
```
